32 devices in a mesh: sp: 8 (over z, x), tp: 4 (over y, core).
Axes of the slice: x: 2, y: 2, z: 4, core: 2. Of those that a mesh axis runs over, the one named last changes fastest.
Arguments:
- residual: bfloat16 [6144, 2048], P('sp'), may hold values from -6 to 6
- queries: bfloat16 [6144, 1024], P('sp', 'tp'), may hold values from -12 to 12
- keys: bfloat16 [6144, 512], P('sp', 'tp'), may hold values from -6 to 6
- values: bfloat16 [6144, 512], P('sp', 'tp'), may hold values from -36 to 36
- segments: int32 [6144], P('sp'), may hold values from 0 to 3, never falling along the last dimension, each value on 1 to 3072 neighbouring positions
- sink: float32 [16], P('tp'), may hold values from 3 to 7
- out_weight: bfloat16 [1024, 2048], replicated, may hold values from -0.1875 to 0.1875
- norm_gain_one: float32 [2048], replicated, may hold values from 0.1 to 1.9
- group: int32 [6144], P('sp'), may hold values from 0 to 3, as said below
- member: int32 [6144, 2], P('sp'), may hold values from 0 to 7, as said below
- route_weight: float32 [6144, 2], P('sp'), may hold values from 0.25 to 1
- gate_weight: bfloat16 [32, 2048, 1024], P('sp', None, 'tp'), may hold values from -0.125 to 0.125
- up_weight: bfloat16 [32, 2048, 1024], P('sp', None, 'tp'), may hold values from -0.125 to 0.125
- down_weight: bfloat16 [32, 1024, 2048], P('sp', None, 'tp'), may hold values from -0.1875 to 0.1875
- norm_gain_two: float32 [2048], P('tp'), may hold values from 0.1 to 1.9
Outputs:
- output: bfloat16 [6144, 2048], P('sp', 'tp')
The draws below stay inside these ranges and needn't reach their ends.
Inputs may be any that keep to these rules, and one draw needn't show every extreme that they name: In every aligned block of 192 rows no expert (group * 8 + member) is named by more than 24 rows, and one expert, the same in all blocks of a draw, is named by exactly 24 rows of every block. `member`: the 2 members of a row differ.
All inputs are finite; a program needn't handle non-finite values.
Results may differ from the reference program's by a relative error of at most 0.0059.
Values may be sent and summed in bfloat16 or wider, within the bound.
A program may use at most 128 MiB of HBM per device.

```python
import math
import jax
import jax.numpy as jnp
import numpy as np
from jax import lax

D = 2048
HEADS = 16
KV_HEADS = 8
HEAD_DIM = 64
HALF = 128
FF = 1024
GROUPS = 4
PER_GROUP = 8
TOP = 2
TOK_DEV = 768
TOKENS = 6144
EXPERTS = 32
BLOCK = 192
CAP = 24
N_SP = 8


def attention_inputs(key):
    parts = jax.random.split(key, 2)
    query_out = jnp.clip(jax.random.normal(parts[0], (TOKENS, HEADS * HEAD_DIM), jnp.float32), -6.0, 6.0)
    key_out = jnp.clip(jax.random.normal(parts[1], (TOKENS, KV_HEADS * HEAD_DIM), jnp.float32), -6.0, 6.0)
    return (query_out, key_out)


def draw_queries(key, part):
    return attention_inputs(jax.random.fold_in(key, 11))[0].astype(jnp.bfloat16)


def draw_keys(key, part):
    return attention_inputs(jax.random.fold_in(key, 11))[1].astype(jnp.bfloat16)


def routing(key):
    blocks = TOKENS // BLOCK
    parts = jax.random.split(key, 6)
    hot_expert = jax.random.randint(parts[0], (), 0, GROUPS * PER_GROUP)
    hot_group = hot_expert // PER_GROUP
    hot_member = hot_expert % PER_GROUP
    scores = jax.random.randint(parts[1], (blocks, BLOCK), 0, 1 << 20) * BLOCK + jnp.arange(BLOCK)[None, :]
    rank = jnp.argsort(jnp.argsort(scores, axis=1, stable=True), axis=1, stable=True).astype(jnp.int32)
    shift_hot = jax.random.randint(parts[2], (blocks, 1), 0, PER_GROUP - 1)
    shift_group = jax.random.randint(parts[3], (blocks, 1), 0, GROUPS - 1)
    offset_table = jax.random.randint(parts[4], (blocks, GROUPS - 1), 0, PER_GROUP)
    gap_table = jax.random.randint(parts[5], (blocks, GROUPS - 1), 0, PER_GROUP - 1)
    is_hot = rank < CAP
    hot_second = (hot_member + 1 + (rank + shift_hot) % (PER_GROUP - 1)) % PER_GROUP
    remainder = jnp.maximum(rank - CAP, 0)
    group_slot = (remainder + shift_group) % (GROUPS - 1)
    other_group = (hot_group + 1 + group_slot) % GROUPS
    cycle_turn = remainder // (GROUPS - 1)
    slot_offset = jnp.take_along_axis(offset_table, group_slot, axis=1)
    slot_gap = jnp.take_along_axis(gap_table, group_slot, axis=1)
    first_member = (cycle_turn + slot_offset) % PER_GROUP
    second_member = (first_member + 1 + slot_gap) % PER_GROUP
    group_out = jnp.where(is_hot, hot_group, other_group).reshape(-1)
    member_one = jnp.where(is_hot, hot_member, first_member).reshape(-1)
    member_two = jnp.where(is_hot, hot_second, second_member).reshape(-1)
    return (group_out.astype(jnp.int32), jnp.stack([member_one, member_two], 1).astype(jnp.int32))


def draw_group(key, part):
    return routing(jax.random.fold_in(key, 23))[0]


def draw_member(key, part):
    return routing(jax.random.fold_in(key, 23))[1]


def levels(own_key, dims, cuts, smallest, largest):
    factor_of = 1.0
    for position, blocks in cuts:
        steps = jax.random.uniform(jax.random.fold_in(jax.random.fold_in(own_key, 6), position), (blocks,), jnp.float32, smallest / len(cuts), largest / len(cuts))
        factor_of = factor_of * jnp.repeat(jnp.exp(steps), dims[position] // blocks).reshape((-1,) + (1,) * (len(dims) - 1 - position))
    return factor_of


def profile(amount, total, limit, slope):
    weights = [(1 << 20) // math.isqrt(grade ** slope) + 1 for grade in range(2, amount + 1)]
    surplus, holding = total - limit - (amount - 1), [1] * (amount - 1)
    while surplus > 0:
        movable = [i for i in range(amount - 1) if holding[i] < limit]
        whole, left = sum([weights[i] for i in movable]), surplus
        for i in movable:
            addition = min(limit - holding[i], max(1, left * weights[i] // whole), surplus)
            holding[i] = holding[i] + addition
            surplus = surplus - addition
    return np.array([limit] + holding)


def ragged_sizes(key, number_of, total, bound, slope):
    if number_of == 2:
        one = jax.random.randint(key, (), max(1, total - bound), min(bound, total - 1) + 1)
        return jnp.stack([one, total - one])
    lengths = jnp.asarray(profile(number_of, total, bound, slope), jnp.int32)
    twos = (number_of - 1) // 2
    giver, receiver = lengths[1:1 + 2 * twos:2], lengths[2:2 + 2 * twos:2]
    room = jnp.minimum(giver - 1, bound - receiver)
    shifted = jax.random.randint(jax.random.fold_in(key, 1), (twos,), 0, 1 << 20) % (room + 1)
    lengths = lengths.at[1:1 + 2 * twos:2].set(giver - shifted).at[2:2 + 2 * twos:2].set(receiver + shifted)
    return lengths[jax.random.permutation(jax.random.fold_in(key, 2), number_of)]


def scatter_about(rng, extent, deviation, most, cuts=(), held_as=jnp.bfloat16):
    factor_of = levels(rng, extent, cuts, -0.22, 0.18) if cuts else 1.0
    entries = jax.random.normal(rng, extent, jnp.float32) * deviation * factor_of
    return jnp.minimum(jnp.maximum(entries, -most), most).astype(held_as)


def setup_inputs(seed: int = 0) -> dict:
    splits = jax.random.split(jax.random.key(seed), 16)
    return {
        "residual": scatter_about(splits[0], (TOKENS, D), 1.0, 6.0, ((0, 8),)),
        "queries": draw_queries(jax.random.fold_in(splits[15], 71), 0),
        "keys": draw_keys(jax.random.fold_in(splits[15], 71), 0),
        "values": scatter_about(splits[3], (TOKENS, KV_HEADS * HEAD_DIM), 6.0, 36.0, ((0, 8), (1, 4))),
        "segments": jnp.searchsorted(jnp.cumsum(ragged_sizes(splits[4], N_SP // 2, TOKENS, 4 * TOK_DEV, 1)), jnp.arange(TOKENS), side="right").astype(jnp.int32),
        "sink": jnp.clip(3.0 + 4.0 * jax.random.uniform(splits[5], (HEADS,), jnp.float32) ** levels(splits[5], (HEADS,), ((0, 4),), -0.2, 0.2), 3.0, 7.0),
        "out_weight": scatter_about(splits[6], (HEADS * HEAD_DIM, D), (HEADS * HEAD_DIM) ** -0.5, 0.1875),
        "norm_gain_one": jnp.clip(1.0 + 0.18 * jax.random.normal(splits[7], (D,), jnp.float32), 0.1, 1.9),
        "group": draw_group(jax.random.fold_in(splits[15], 71), 0),
        "member": draw_member(jax.random.fold_in(splits[15], 71), 0),
        "route_weight": jnp.clip(jnp.exp(math.log(1.0) - 1.3862944 * jax.random.uniform(splits[10], (TOKENS, TOP), jnp.float32) ** levels(splits[10], (TOKENS, TOP), ((0, 8),), -0.2, 0.2)), 0.25, 1.0),
        "gate_weight": scatter_about(splits[11], (EXPERTS, D, FF), D ** -0.5, 0.125, ((0, 8), (2, 4))),
        "up_weight": scatter_about(splits[12], (EXPERTS, D, FF), D ** -0.5, 0.125, ((0, 8), (2, 4))),
        "down_weight": scatter_about(splits[13], (EXPERTS, FF, D), FF ** -0.5, 0.1875, ((0, 8), (2, 4))),
        "norm_gain_two": jnp.clip(1.0 + 0.18 * jax.random.normal(splits[14], (D,), jnp.float32), 0.1, 1.9),
    }


ALPHA = 2.0 ** 0.25
EPS = 1e-05

def layer_norm(summed, norm_gain):
    mean_value = lax.optimization_barrier(jnp.mean(summed, -1, keepdims=True))
    variance = lax.optimization_barrier(jnp.mean(jnp.square(summed - mean_value), -1, keepdims=True))
    return ((summed - mean_value) * lax.rsqrt(variance + EPS) * norm_gain).astype(jnp.bfloat16)

def reference(residual, queries, keys, values, segments, sink, out_weight, norm_gain_one, group, member, route_weight, gate_weight, up_weight, down_weight, norm_gain_two):
    seq_total = queries.shape[0]
    group_size = HEADS // KV_HEADS
    query_block = math.gcd(seq_total, 512)
    key_span = query_block + 2 * HALF
    query_heads = queries.reshape(seq_total, KV_HEADS, group_size, HEAD_DIM)
    key_padded = jnp.pad(keys, ((HALF, HALF), (0, 0))).reshape(seq_total + 2 * HALF, KV_HEADS, HEAD_DIM)
    value_padded = jnp.pad(values, ((HALF, HALF), (0, 0))).reshape(seq_total + 2 * HALF, KV_HEADS, HEAD_DIM)
    seg_padded = jnp.pad(segments, (HALF, HALF), constant_values=-1)
    offsets = jnp.arange(key_span)[None, :] - HALF - jnp.arange(query_block)[:, None]
    in_band = jnp.abs(offsets) <= HALF
    sink_heads = sink.astype(jnp.float32).reshape(KV_HEADS, group_size, 1, 1)

    def attend(number):
        row_low = (number * query_block).astype(jnp.int32)
        query_rows = lax.dynamic_slice_in_dim(query_heads, row_low, query_block, 0)
        key_part = lax.dynamic_slice_in_dim(key_padded, row_low, key_span, 0)
        value_part = lax.dynamic_slice_in_dim(value_padded, row_low, key_span, 0)
        seg_query = lax.dynamic_slice_in_dim(segments, row_low, query_block, 0)
        seg_keys = lax.dynamic_slice_in_dim(seg_padded, row_low, key_span, 0)
        allowed = in_band & (seg_query[:, None] == seg_keys[None, :])
        scores = jnp.einsum('qkgd,ckd->kgqc', query_rows.astype(jnp.float32), key_part.astype(jnp.float32)) * HEAD_DIM ** (-0.5)
        masked = jnp.where(allowed, scores, -1e+30)
        peak = jnp.maximum(lax.optimization_barrier(jnp.max(masked, -1, keepdims=True)), sink_heads)
        raised = jnp.where(allowed, jnp.exp(masked - peak), 0.0)
        denominator = lax.optimization_barrier(jnp.sum(raised, -1, keepdims=True)) + jnp.exp(sink_heads - peak)
        weights = (raised / denominator).astype(jnp.bfloat16)
        attended_part = jnp.einsum('kgqc,ckd->qkgd', weights.astype(jnp.float32), value_part.astype(jnp.float32))
        return attended_part.reshape(query_block, HEADS * HEAD_DIM).astype(jnp.bfloat16)
    attended = lax.map(attend, jnp.arange(seq_total // query_block, dtype=jnp.int32)).reshape(seq_total, HEADS * HEAD_DIM)
    mixed = jnp.dot(attended, out_weight, preferred_element_type=jnp.float32)
    pre_one = ALPHA * residual.astype(jnp.float32) + mixed
    normed = layer_norm(pre_one, norm_gain_one.astype(jnp.float32))
    copies = seq_total * TOP
    flat_expert = (group[:, None] * PER_GROUP + member).reshape(-1).astype(jnp.int32)
    normed_ext = jnp.concatenate([normed, jnp.zeros((1, D), jnp.bfloat16)], 0)
    capacity_all = CAP * (TOKENS // BLOCK)

    def expert_rows(expert):
        copy_index = jnp.nonzero(flat_expert == expert, size=capacity_all, fill_value=copies)[0].astype(jnp.int32)
        taken = normed_ext[copy_index // TOP]
        gate_part = jnp.dot(taken, gate_weight[expert], preferred_element_type=jnp.float32)
        up_part = jnp.dot(taken, up_weight[expert], preferred_element_type=jnp.float32)
        hidden = (jax.nn.silu(gate_part) * up_part).astype(jnp.bfloat16)
        result = jnp.dot(hidden, down_weight[expert], preferred_element_type=jnp.float32).astype(jnp.bfloat16)
        return (copy_index, result)
    indices, results = lax.map(expert_rows, jnp.arange(EXPERTS, dtype=jnp.int32))
    per_copy = jnp.zeros((copies + 1, D), jnp.bfloat16).at[indices.reshape(-1)].set(results.reshape(-1, D))
    per_copy = per_copy[:copies].reshape(seq_total, TOP, D)
    combined = lax.optimization_barrier(jnp.sum(route_weight.astype(jnp.float32)[:, :, None] * per_copy.astype(jnp.float32), 1))
    pre_two = ALPHA * normed.astype(jnp.float32) + combined
    return layer_norm(pre_two, norm_gain_two.astype(jnp.float32))
```

```python
import functools
import math

import jax
import jax.numpy as jnp
from jax import lax
from jax.experimental import pallas as pl
from jax.experimental.pallas import tpu as pltpu
from jax.sharding import PartitionSpec as P

HEAD_DIM = 64
HALF = 128
PER_GROUP = 8


ALPHA = 2.0**0.25
EPS = 1e-05


def with_halo(block, sides, width):
    for axis, dim in sides:
        count = lax.axis_size(axis)
        forward = [(i, i + 1) for i in range(count - 1)]
        backward = [(target, source) for source, target in forward]
        low = lax.ppermute(
            lax.slice_in_dim(block, block.shape[dim] - width, None, axis=dim), axis, forward
        )
        high = lax.ppermute(lax.slice_in_dim(block, 0, width, axis=dim), axis, backward)
        block = jnp.concatenate([low, block, high], axis=dim)
    return block


def layer_norm(summed, norm_gain):
    mean_value = jnp.mean(summed, -1, keepdims=True)
    variance = jnp.mean(jnp.square(summed - mean_value), -1, keepdims=True)
    return ((summed - mean_value) * lax.rsqrt(variance + EPS) * norm_gain).astype(jnp.bfloat16)


MESH = pl.DeviceIdType.MESH


def expert_kernel(
    groups,
    out_ref,
    pick_ref,
    join_ref,
    gate_hbm,
    up_hbm,
    down_hbm,
    result_ref,
    rows,
    taken,
    gate,
    up,
    down,
    hidden,
    made,
    kept,
    across,
    beside,
    summed,
    back,
    weight_sem,
    place_sem,
    send_sem,
    recv_sem,
):
    sp = lax.axis_index("sp")
    tp = lax.axis_index("tp")
    z, x = sp // 2, sp % 2
    y, c = tp // 2, tp % 2
    room = out_ref.shape[1]
    experts = gate.shape[0]
    first = room // 2 // 16 * 16

    load_gate = pltpu.make_async_copy(gate_hbm, gate, weight_sem.at[0])
    load_up = pltpu.make_async_copy(up_hbm, up, weight_sem.at[1])
    load_down = pltpu.make_async_copy(down_hbm, down, weight_sem.at[2])
    load_gate.start()
    load_up.start()
    load_down.start()

    beside_x = (z * 2 + 1 - x, tp)
    beside_y = (sp, (1 - y) * 2 + c)
    sibling = (sp, y * 2 + 1 - c)
    far = [(lax.rem(z + k, groups) * 2 + x, tp) for k in range(1, groups)]
    barrier = pltpu.get_barrier_semaphore()
    for device in [beside_x, beside_y, sibling] + far:
        pl.semaphore_signal(barrier, inc=1, device_id=device, device_id_type=MESH)
    pl.semaphore_wait(barrier, groups + 2)

    def place(zs, xs, ys, cs, low=0, size=None):
        size = room if size is None else size
        start = pl.multiple_of(cs * room + low, 16)
        return rows.at[(zs * 2 + xs) * 2 + ys, pl.ds(start, size)]

    def copy(ref, device, kind, k, source=None):
        return pltpu.make_async_remote_copy(
            src_ref=ref if source is None else source,
            dst_ref=ref,
            send_sem=send_sem.at[kind, k],
            recv_sem=recv_sem.at[kind, k],
            device_id=device,
            device_id_type=MESH,
        )

    started = []

    def send(*args, **named):
        one = copy(*args, **named)
        one.start()
        started.append(one)

    def arrive(ref, kind, k):
        copy(ref, sibling, kind, k).wait_recv()

    own = pltpu.make_async_copy(out_ref.at[z], place(z, x, y, c), place_sem)
    own.start()
    for k in range(1, groups):
        send(place(z, x, y, c), far[k - 1], 0, k, source=out_ref.at[lax.rem(z + k, groups)])
    own.wait()
    sources = [lax.rem(z + groups - k, groups) for k in range(groups)]

    def begin(k):
        zs = sources[k]
        if k:
            arrive(place(zs, x, y, c), 0, k)
        send(place(zs, x, y, c), beside_x, 1, k)
        send(place(zs, x, y, c), beside_y, 2, k)
        send(place(zs, x, y, c), sibling, 3, k)

    def forward(k):
        zs = sources[k]
        arrive(place(zs, 1 - x, y, c), 1, k)
        send(place(zs, 1 - x, y, c, 0, first), beside_y, 4, k)
        send(place(zs, 1 - x, y, c), sibling, 6, k)
        arrive(place(zs, x, 1 - y, c), 2, k)
        send(place(zs, x, 1 - y, c, first, room - first), beside_x, 5, k)
        send(place(zs, x, 1 - y, c), sibling, 7, k)

    def finish(k):
        zs = sources[k]
        arrive(place(zs, 1 - x, 1 - y, c, 0, first), 4, k)
        send(place(zs, 1 - x, 1 - y, c, 0, first), sibling, 8, k)
        arrive(place(zs, 1 - x, 1 - y, c, first, room - first), 5, k)
        send(place(zs, 1 - x, 1 - y, c, first, room - first), sibling, 9, k)
        arrive(place(zs, x, y, 1 - c), 3, k)
        arrive(place(zs, 1 - x, y, 1 - c), 6, k)
        arrive(place(zs, x, 1 - y, 1 - c), 7, k)
        arrive(place(zs, 1 - x, 1 - y, 1 - c, 0, first), 8, k)
        arrive(place(zs, 1 - x, 1 - y, 1 - c, first, room - first), 9, k)

    pair_rows = pick_ref.shape[1] // experts

    def compute(k):
        zs = sources[k]
        for pair in range(4):
            chosen = jnp.dot(
                pick_ref[zs * 4 + pair], rows[zs * 4 + pair], preferred_element_type=jnp.float32
            ).astype(jnp.bfloat16)
            for e in range(experts):
                taken[e, pair * pair_rows : (pair + 1) * pair_rows, :] = chosen[
                    e * pair_rows : (e + 1) * pair_rows
                ]

        def one(e, carry):
            gate_part = jnp.dot(taken[e], gate[e], preferred_element_type=jnp.float32)
            up_part = jnp.dot(taken[e], up[e], preferred_element_type=jnp.float32)
            silu = gate_part / (1.0 + jnp.exp(-gate_part))
            hidden[zs, tp, e] = (silu * up_part).astype(jnp.bfloat16)
            return carry

        lax.fori_loop(0, experts, one, 0)
        send(hidden.at[zs, tp], beside_y, 10, k)
        send(hidden.at[zs, tp], sibling, 11, k)

    def share(k):
        other = hidden.at[sources[k], (1 - y) * 2 + c]
        arrive(other, 10, k)
        send(other, sibling, 12, k)

    part = down.shape[1] // 4

    def project(k):
        zs = sources[k]
        arrive(hidden.at[zs, y * 2 + 1 - c], 11, k)
        arrive(hidden.at[zs, (1 - y) * 2 + 1 - c], 12, k)
        if k == 0:
            load_down.wait()

        def one(e, carry):
            total = jnp.dot(
                hidden[zs, 0, e], down[e, :part, :], preferred_element_type=jnp.float32
            )
            for t in range(1, 4):
                total += jnp.dot(
                    hidden[zs, t, e],
                    down[e, t * part : (t + 1) * part, :],
                    preferred_element_type=jnp.float32,
                )
            total = total.astype(jnp.bfloat16)
            start = pl.multiple_of(e * pair_rows, 16)
            for pair in range(4):
                made[pair, pl.ds(start, pair_rows), :] = total[
                    pair * pair_rows : (pair + 1) * pair_rows
                ]
            return carry

        lax.fori_loop(0, experts, one, 0)

        def joined(xs, ys):
            at = zs * 4 + xs * 2 + ys
            slots = made[xs * 2 + ys]
            return jnp.dot(
                join_ref[0, at], slots, preferred_element_type=jnp.float32
            ) + jnp.dot(join_ref[1, at], slots, preferred_element_type=jnp.float32)

        for ys in range(2):
            across[zs, ys] = joined(1 - x, ys).astype(jnp.bfloat16)
        send(beside.at[zs], beside_x, 13, k, source=across.at[zs])
        for ys in range(2):
            kept[k % 2, ys] = joined(x, ys)

    def give(k):
        zs = sources[k]
        arrive(beside.at[zs], 13, k)
        total = (kept[k % 2] + beside[zs].astype(jnp.float32)).astype(jnp.bfloat16)
        if k == 0:
            back[z] = total
        else:
            summed[k] = total
            send(back.at[z], (zs * 2 + x, tp), 14, k, source=summed.at[k])

    for k in range(groups + 3):
        if k < groups:
            begin(k)
        if 0 < k <= groups:
            finish(k - 1)
            if k == 1:
                load_gate.wait()
                load_up.wait()
            compute(k - 1)
        if k < groups:
            forward(k)
        if 0 < k <= groups:
            share(k - 1)
        if 0 <= k - 2 < groups:
            project(k - 2)
        if 0 <= k - 3 < groups:
            give(k - 3)
    for k in range(1, groups):
        arrive(back.at[lax.rem(z + k, groups)], 14, k)
    result_ref[...] = back[...]
    for one in started:
        one.wait_send()


def group_experts(outgoing, picks, joins, gate_weight, up_weight, down_weight):
    groups, room, width = outgoing.shape
    experts, _, hidden_width = gate_weight.shape
    pairs, pair_slots, pair_rows = picks.shape
    chunk = pair_slots // experts * 4
    out_width = down_weight.shape[2]
    part = (groups, 2, pair_rows, out_width)
    return pl.pallas_call(
        functools.partial(expert_kernel, groups),
        out_shape=jax.ShapeDtypeStruct(part, jnp.bfloat16),
        in_specs=[
            pl.BlockSpec(memory_space=pltpu.VMEM),
            pl.BlockSpec(memory_space=pltpu.VMEM),
            pl.BlockSpec(memory_space=pltpu.VMEM),
            pl.BlockSpec(memory_space=pl.ANY),
            pl.BlockSpec(memory_space=pl.ANY),
            pl.BlockSpec(memory_space=pl.ANY),
        ],
        out_specs=pl.BlockSpec(memory_space=pltpu.VMEM),
        scratch_shapes=[
            pltpu.VMEM((pairs, pair_rows, width), jnp.bfloat16),
            pltpu.VMEM((experts, chunk, width), jnp.bfloat16),
            pltpu.VMEM(gate_weight.shape, jnp.bfloat16),
            pltpu.VMEM(up_weight.shape, jnp.bfloat16),
            pltpu.VMEM(down_weight.shape, jnp.bfloat16),
            pltpu.VMEM((groups, 4, experts, chunk, hidden_width), jnp.bfloat16),
            pltpu.VMEM((4, pair_slots, out_width), jnp.bfloat16),
            pltpu.VMEM((2,) + part[1:], jnp.float32),
            pltpu.VMEM(part, jnp.bfloat16),
            pltpu.VMEM(part, jnp.bfloat16),
            pltpu.VMEM(part, jnp.bfloat16),
            pltpu.VMEM(part, jnp.bfloat16),
            pltpu.SemaphoreType.DMA((3,)),
            pltpu.SemaphoreType.DMA,
            pltpu.SemaphoreType.DMA((15, groups)),
            pltpu.SemaphoreType.DMA((15, groups)),
        ],
        compiler_params=pltpu.CompilerParams(
            collective_id=0, has_side_effects=True, vmem_limit_bytes=63 * 1024 * 1024
        ),
    )(outgoing, picks, joins, gate_weight, up_weight, down_weight)


def group_ranks(mine):
    count = mine.astype(jnp.int32)
    return jnp.cumsum(count, 1) - count


def experts_by_group(
    normed, group, member, route_weight, gate_weight, up_weight, down_weight, capacity
):
    sp_size, tp_size = lax.axis_size("sp"), lax.axis_size("tp")
    row_count = normed.shape[0]
    block_rows = row_count // tp_size
    experts_local = gate_weight.shape[0]
    groups = experts_local * sp_size // PER_GROUP
    room = capacity * PER_GROUP // member.shape[1]
    packed = (group * PER_GROUP + member[:, 0]) * PER_GROUP + member[:, 1]
    every = lax.all_gather(packed, "sp", axis=0, tiled=True).reshape(-1, block_rows)
    own_group = lax.axis_index("sp") * experts_local // PER_GROUP
    first_expert = lax.axis_index("sp") * experts_local % PER_GROUP
    mine = every // (PER_GROUP * PER_GROUP) == own_group
    at = group_ranks(mine)
    names = [every // PER_GROUP % PER_GROUP, every % PER_GROUP]
    local = first_expert + jnp.arange(experts_local)[None, :, None]
    named = ((names[0][:, None, :] == local) | (names[1][:, None, :] == local)) & mine[:, None, :]
    slot = jnp.cumsum(named.astype(jnp.int32), 2) - 1
    slot = jnp.where(named, slot, -1)
    blocks = every.shape[0]
    slot_hot = (slot[:, :, None, :] == jnp.arange(capacity)[None, None, :, None]).astype(jnp.bfloat16)
    row_hot = (
        (at[:, :, None] == jnp.arange(room)[None, None, :]) & mine[:, :, None]
    ).astype(jnp.bfloat16)
    pick = jnp.einsum(
        "bsr,brg->bsg",
        slot_hot.reshape(blocks, experts_local * capacity, block_rows),
        row_hot,
        preferred_element_type=jnp.float32,
    ).astype(jnp.bfloat16)
    pick = pick.reshape(blocks // 2, 2, experts_local, capacity, room).transpose(0, 2, 1, 3, 4)
    both = jnp.eye(2, dtype=jnp.bfloat16)[None, None, :, None, :, None] * pick[:, :, :, :, None, :]
    picks = both.reshape(blocks // 2, experts_local * 2 * capacity, 2 * room)
    routes = lax.all_gather(route_weight.T, "sp", axis=1, tiled=True)
    routes = routes.reshape(2, blocks, 1, block_rows)
    routed = jnp.where(names[0][:, None, :] == local, routes[0], routes[1])
    slot_weight = jnp.sum(slot_hot.astype(jnp.float32) * routed[:, :, None, :], 3)
    slot_weight = slot_weight.reshape(blocks // 2, 2, experts_local, capacity)
    slot_weight = slot_weight.transpose(0, 2, 1, 3).reshape(blocks // 2, 1, -1)
    coarse = slot_weight.astype(jnp.bfloat16)
    fine = (slot_weight - coarse.astype(jnp.float32)).astype(jnp.bfloat16)
    joins = picks.transpose(0, 2, 1)[None] * jnp.stack([coarse, fine])
    by_block = group.reshape(tp_size, block_rows)
    group_mask = by_block[:, None, :] == jnp.arange(groups)[None, :, None]
    count = group_mask.astype(jnp.int32)
    place = jnp.cumsum(count, 2) - count
    choose = (
        (place[:, :, None, :] == jnp.arange(room)[None, None, :, None]) & group_mask[:, :, None, :]
    ).astype(jnp.bfloat16)
    choose = choose.reshape(tp_size, groups * room, block_rows)
    own_choose = lax.dynamic_index_in_dim(choose, lax.axis_index("tp"), 0, keepdims=False)
    own_rows = lax.dynamic_slice_in_dim(normed, lax.axis_index("tp") * block_rows, block_rows, 0)
    outgoing = jnp.dot(own_choose, own_rows, preferred_element_type=jnp.float32)
    outgoing = outgoing.astype(jnp.bfloat16).reshape(groups, room, normed.shape[1])
    back = group_experts(outgoing, picks, joins, gate_weight, up_weight, down_weight)
    back = back.reshape(groups, tp_size, room, -1).transpose(1, 0, 2, 3)
    back = back.reshape(tp_size, groups * room, -1)
    combined = jnp.einsum("tgr,tgc->trc", choose, back, preferred_element_type=jnp.float32)
    return combined.reshape(row_count, -1)


def shards(
    residual,
    queries,
    keys,
    values,
    segments,
    sink,
    out_weight,
    norm_gain_one,
    group,
    member,
    route_weight,
    gate_weight,
    up_weight,
    down_weight,
    norm_gain_two,
):
    row_count = queries.shape[0]
    sp_size = lax.axis_size("sp")
    tp_size = lax.axis_size("tp")
    kv_local = keys.shape[1] // HEAD_DIM
    heads_local = queries.shape[1] // HEAD_DIM
    group_size = heads_local // kv_local
    seq_total = row_count * sp_size
    seq_start = lax.axis_index("sp") * row_count
    joined = jnp.concatenate([keys, values], axis=1)
    padded, seg_padded = (
        with_halo(joined, (("sp", 0),), HALF),
        with_halo(segments, (("sp", 0),), HALF),
    )
    query_block = math.gcd(row_count, 512)
    key_span = query_block + 2 * HALF
    offsets = jnp.arange(key_span)[None, :] - HALF - jnp.arange(query_block)[:, None]
    in_band = jnp.abs(offsets) <= HALF
    sink_heads = sink.reshape(kv_local, group_size, 1, 1)
    query_heads = queries.reshape(row_count, kv_local, group_size, HEAD_DIM)
    key_cols = kv_local * HEAD_DIM
    pieces = []
    for number in range(row_count // query_block):
        row_low = number * query_block
        query_rows = query_heads[row_low : row_low + query_block]
        kv_rows = padded[row_low : row_low + key_span]
        key_part = kv_rows[:, :key_cols].reshape(key_span, kv_local, HEAD_DIM)
        value_part = kv_rows[:, key_cols:].reshape(key_span, kv_local, HEAD_DIM)
        key_place = seq_start + row_low - HALF + jnp.arange(key_span)
        inside = (key_place >= 0) & (key_place < seq_total)
        same_doc = (
            segments[row_low : row_low + query_block, None]
            == seg_padded[None, row_low : row_low + key_span]
        )
        allowed = in_band & same_doc & inside[None, :]
        scores = jnp.einsum(
            "qkgd,ckd->kgqc", query_rows, key_part, preferred_element_type=jnp.float32
        ) * HEAD_DIM ** (-0.5)
        masked = jnp.where(allowed, scores, -1e30)
        peak = jnp.maximum(jnp.max(masked, -1, keepdims=True), sink_heads)
        raised = jnp.where(allowed, jnp.exp(masked - peak), 0.0)
        denominator = jnp.sum(raised, -1, keepdims=True) + jnp.exp(sink_heads - peak)
        weights = (raised / denominator).astype(jnp.bfloat16)
        attended_part = jnp.einsum(
            "kgqc,ckd->qkgd", weights, value_part, preferred_element_type=jnp.float32
        )
        pieces.append(
            attended_part.reshape(query_block, heads_local * HEAD_DIM).astype(jnp.bfloat16)
        )
    attended = jnp.concatenate(pieces, 0)
    width = out_weight.shape[1]
    weight_rows = out_weight
    mixed = jnp.dot(
        lax.all_gather(attended, "tp", axis=1, tiled=True),
        weight_rows,
        preferred_element_type=jnp.float32,
    )
    pre_one = ALPHA * residual.astype(jnp.float32) + mixed
    normed = layer_norm(pre_one, norm_gain_one)
    experts_local = gate_weight.shape[0]
    expert_count = experts_local * sp_size
    picks_count = member.shape[1]
    block_rows = row_count // tp_size
    capacity = max(2, block_rows // 8)
    column_width = down_weight.shape[2]
    if experts_local * 2 == PER_GROUP and tp_size == 4:
        combined = experts_by_group(
            normed, group, member, route_weight, gate_weight, up_weight, down_weight, capacity
        )
    else:
        expert_ids = (group[:, None] * PER_GROUP + member).reshape(tp_size, block_rows * picks_count)
        onehot_table = (expert_ids[:, :, None] == jnp.arange(expert_count)[None, None, :]).astype(
            jnp.int32
        )
        ranks = jnp.sum((jnp.cumsum(onehot_table, 1) - 1) * onehot_table, 2)
        owner = expert_ids // experts_local
        local_ids = expert_ids % experts_local
        block_ids = jnp.arange(tp_size)[:, None]
        slot_all = ((local_ids * sp_size + owner) * tp_size + block_ids) * capacity + ranks
        copy_rows = (
            jnp.arange(row_count * picks_count).reshape(tp_size, block_rows * picks_count)
            // picks_count
        )
        extended = jnp.concatenate([normed, jnp.zeros((1, width), jnp.bfloat16)], 0)
        tp_place = lax.axis_index("tp")
        slot_own_base = (local_ids * sp_size + owner) * capacity + ranks
        own_slots = lax.dynamic_index_in_dim(slot_own_base, tp_place, 0, keepdims=False)
        own_rows = lax.dynamic_index_in_dim(copy_rows, tp_place, 0, keepdims=False)
        slot_count = experts_local * sp_size * capacity
        source = jnp.full((slot_count,), row_count, jnp.int32).at[own_slots].set(own_rows)
        outgoing = extended[source].reshape(experts_local, sp_size, capacity, width)
        received = lax.all_to_all(outgoing, "sp", split_axis=1, concat_axis=1, tiled=True)
        arrived = lax.all_gather(received, "tp", axis=2, tiled=True)
        expert_rows = arrived.reshape(experts_local, sp_size * tp_size * capacity, width)
        gate_part = jnp.einsum(
            "esd,edf->esf", expert_rows, gate_weight, preferred_element_type=jnp.float32
        )
        up_part = jnp.einsum("esd,edf->esf", expert_rows, up_weight, preferred_element_type=jnp.float32)
        hidden = (jax.nn.silu(gate_part) * up_part).astype(jnp.bfloat16)
        weight_rows = down_weight
        produced = jnp.einsum(
            "esf,efc->esc",
            lax.all_gather(hidden, "tp", axis=2, tiled=True),
            weight_rows,
            preferred_element_type=jnp.float32,
        ).astype(jnp.bfloat16)
        returned = lax.all_to_all(
            produced.reshape(experts_local, sp_size, tp_size * capacity, column_width),
            "sp",
            split_axis=1,
            concat_axis=1,
            tiled=True,
        )
        result_rows = returned.reshape(-1, column_width)
        picked = result_rows[slot_all.reshape(row_count, picks_count)]
        combined = jnp.sum(route_weight[:, :, None] * picked.astype(jnp.float32), 1)
    column_start = lax.axis_index("tp") * column_width
    normed_part = lax.dynamic_slice_in_dim(normed, column_start, column_width, 1)
    pre_two = ALPHA * normed_part.astype(jnp.float32) + combined
    sums, squares = lax.psum((jnp.sum(pre_two, -1), jnp.sum(pre_two * pre_two, -1)), "tp")
    mean_value = (sums / width)[:, None]
    variance = (squares / width)[:, None] - mean_value * mean_value
    return ((pre_two - mean_value) * lax.rsqrt(variance + EPS) * norm_gain_two).astype(jnp.bfloat16)


def solution(mesh):
    in_specs = (
        P("sp", None),
        P("sp", "tp"),
        P("sp", "tp"),
        P("sp", "tp"),
        P("sp"),
        P("tp"),
        P(),
        P(),
        P("sp"),
        P("sp", None),
        P("sp", None),
        P("sp", None, "tp"),
        P("sp", None, "tp"),
        P("sp", None, "tp"),
        P("tp"),
    )
    out_specs = P("sp", "tp")
    return jax.shard_map(shards, mesh=mesh, in_specs=in_specs, out_specs=out_specs, check_vma=False)
```

```python
import functools
import math

import jax
import jax.numpy as jnp
from jax import lax
from jax.experimental import pallas as pl
from jax.experimental.pallas import tpu as pltpu
from jax.sharding import PartitionSpec as P

HEAD_DIM = 64
HALF = 128
PER_GROUP = 8


ALPHA = 2.0**0.25
EPS = 1e-05


def with_halo(block, sides, width):
    for axis, dim in sides:
        count = lax.axis_size(axis)
        forward = [(i, i + 1) for i in range(count - 1)]
        backward = [(target, source) for source, target in forward]
        low = lax.ppermute(
            lax.slice_in_dim(block, block.shape[dim] - width, None, axis=dim), axis, forward
        )
        high = lax.ppermute(lax.slice_in_dim(block, 0, width, axis=dim), axis, backward)
        block = jnp.concatenate([low, block, high], axis=dim)
    return block


def layer_norm(summed, norm_gain):
    mean_value = jnp.mean(summed, -1, keepdims=True)
    variance = jnp.mean(jnp.square(summed - mean_value), -1, keepdims=True)
    return ((summed - mean_value) * lax.rsqrt(variance + EPS) * norm_gain).astype(jnp.bfloat16)


MESH = pl.DeviceIdType.MESH


def expert_kernel(
    groups,
    out_ref,
    pick_ref,
    join_ref,
    gate_hbm,
    up_hbm,
    down_hbm,
    result_ref,
    rows,
    taken,
    gate,
    up,
    down,
    hidden,
    made,
    kept,
    across,
    beside,
    summed,
    back,
    weight_sem,
    place_sem,
    send_sem,
    recv_sem,
):
    sp = lax.axis_index("sp")
    tp = lax.axis_index("tp")
    z, x = sp // 2, sp % 2
    y, c = tp // 2, tp % 2
    room = out_ref.shape[1]
    experts = gate.shape[0]
    first = room // 2 // 16 * 16

    load_gate = pltpu.make_async_copy(gate_hbm, gate, weight_sem.at[0])
    load_up = pltpu.make_async_copy(up_hbm, up, weight_sem.at[1])
    load_down = pltpu.make_async_copy(down_hbm, down, weight_sem.at[2])
    load_gate.start()
    load_up.start()
    load_down.start()

    beside_x = (z * 2 + 1 - x, tp)
    beside_y = (sp, (1 - y) * 2 + c)
    sibling = (sp, y * 2 + 1 - c)
    far = [(lax.rem(z + k, groups) * 2 + x, tp) for k in range(1, groups)]
    barrier = pltpu.get_barrier_semaphore()
    for device in [beside_x, beside_y, sibling] + far:
        pl.semaphore_signal(barrier, inc=1, device_id=device, device_id_type=MESH)
    pl.semaphore_wait(barrier, groups + 2)

    def place(zs, xs, ys, cs, low=0, size=None):
        size = room if size is None else size
        start = pl.multiple_of(cs * room + low, 16)
        return rows.at[(zs * 2 + xs) * 2 + ys, pl.ds(start, size)]

    def copy(ref, device, kind, k, source=None):
        return pltpu.make_async_remote_copy(
            src_ref=ref if source is None else source,
            dst_ref=ref,
            send_sem=send_sem.at[kind, k],
            recv_sem=recv_sem.at[kind, k],
            device_id=device,
            device_id_type=MESH,
        )

    started = []

    def send(*args, **named):
        one = copy(*args, **named)
        one.start()
        started.append(one)

    def arrive(ref, kind, k):
        copy(ref, sibling, kind, k).wait_recv()

    own = pltpu.make_async_copy(out_ref.at[z], place(z, x, y, c), place_sem)
    own.start()
    for k in range(1, groups):
        send(place(z, x, y, c), far[k - 1], 0, k, source=out_ref.at[lax.rem(z + k, groups)])
    own.wait()
    sources = [lax.rem(z + groups - k, groups) for k in range(groups)]

    def begin(k):
        zs = sources[k]
        if k:
            arrive(place(zs, x, y, c), 0, k)
        send(place(zs, x, y, c), beside_x, 1, k)
        send(place(zs, x, y, c), beside_y, 2, k)
        send(place(zs, x, y, c), sibling, 3, k)

    def forward(k):
        zs = sources[k]
        arrive(place(zs, 1 - x, y, c), 1, k)
        send(place(zs, 1 - x, y, c, 0, first), beside_y, 4, k)
        send(place(zs, 1 - x, y, c), sibling, 6, k)
        arrive(place(zs, x, 1 - y, c), 2, k)
        send(place(zs, x, 1 - y, c, first, room - first), beside_x, 5, k)
        send(place(zs, x, 1 - y, c), sibling, 7, k)

    def finish(k):
        zs = sources[k]
        arrive(place(zs, 1 - x, 1 - y, c, 0, first), 4, k)
        send(place(zs, 1 - x, 1 - y, c, 0, first), sibling, 8, k)
        arrive(place(zs, 1 - x, 1 - y, c, first, room - first), 5, k)
        send(place(zs, 1 - x, 1 - y, c, first, room - first), sibling, 9, k)
        arrive(place(zs, x, y, 1 - c), 3, k)
        arrive(place(zs, 1 - x, y, 1 - c), 6, k)
        arrive(place(zs, x, 1 - y, 1 - c), 7, k)
        arrive(place(zs, 1 - x, 1 - y, 1 - c, 0, first), 8, k)
        arrive(place(zs, 1 - x, 1 - y, 1 - c, first, room - first), 9, k)

    pair_rows = pick_ref.shape[1] // experts

    def compute(k):
        zs = sources[k]
        for pair in range(4):
            chosen = jnp.dot(
                pick_ref[zs * 4 + pair], rows[zs * 4 + pair], preferred_element_type=jnp.float32
            ).astype(jnp.bfloat16)
            for e in range(experts):
                taken[e, pair * pair_rows : (pair + 1) * pair_rows, :] = chosen[
                    e * pair_rows : (e + 1) * pair_rows
                ]

        def one(e, carry):
            gate_part = jnp.dot(taken[e], gate[e], preferred_element_type=jnp.float32)
            up_part = jnp.dot(taken[e], up[e], preferred_element_type=jnp.float32)
            silu = gate_part / (1.0 + jnp.exp(-gate_part))
            hidden[zs, tp, e] = (silu * up_part).astype(jnp.bfloat16)
            return carry

        lax.fori_loop(0, experts, one, 0)
        send(hidden.at[zs, tp], beside_y, 10, k)
        send(hidden.at[zs, tp], sibling, 11, k)

    def share(k):
        other = hidden.at[sources[k], (1 - y) * 2 + c]
        arrive(other, 10, k)
        send(other, sibling, 12, k)

    part = down.shape[1] // 4

    def project(k):
        zs = sources[k]
        arrive(hidden.at[zs, y * 2 + 1 - c], 11, k)
        arrive(hidden.at[zs, (1 - y) * 2 + 1 - c], 12, k)
        if k == 0:
            load_down.wait()

        def one(e, carry):
            total = jnp.dot(
                hidden[zs, 0, e], down[e, :part, :], preferred_element_type=jnp.float32
            )
            for t in range(1, 4):
                total += jnp.dot(
                    hidden[zs, t, e],
                    down[e, t * part : (t + 1) * part, :],
                    preferred_element_type=jnp.float32,
                )
            total = total.astype(jnp.bfloat16)
            start = pl.multiple_of(e * pair_rows, 16)
            for pair in range(4):
                made[pair, pl.ds(start, pair_rows), :] = total[
                    pair * pair_rows : (pair + 1) * pair_rows
                ]
            return carry

        lax.fori_loop(0, experts, one, 0)

        def joined(xs, ys):
            at = zs * 4 + xs * 2 + ys
            slots = made[xs * 2 + ys]
            return jnp.dot(
                join_ref[0, at], slots, preferred_element_type=jnp.float32
            ) + jnp.dot(join_ref[1, at], slots, preferred_element_type=jnp.float32)

        for ys in range(2):
            across[zs, ys] = joined(1 - x, ys).astype(jnp.bfloat16)
        send(beside.at[zs], beside_x, 13, k, source=across.at[zs])
        for ys in range(2):
            kept[k % 2, ys] = joined(x, ys)

    def give(k):
        zs = sources[k]
        arrive(beside.at[zs], 13, k)
        total = (kept[k % 2] + beside[zs].astype(jnp.float32)).astype(jnp.bfloat16)
        if k == 0:
            back[z] = total
        else:
            summed[k] = total
            send(back.at[z], (zs * 2 + x, tp), 14, k, source=summed.at[k])

    for k in range(groups + 3):
        if k < groups:
            begin(k)
        if 0 < k <= groups:
            finish(k - 1)
            if k == 1:
                load_gate.wait()
                load_up.wait()
            compute(k - 1)
        if k < groups:
            forward(k)
        if 0 < k <= groups:
            share(k - 1)
        if 0 <= k - 2 < groups:
            project(k - 2)
        if 0 <= k - 3 < groups:
            give(k - 3)
    for k in range(1, groups):
        arrive(back.at[lax.rem(z + k, groups)], 14, k)
    result_ref[...] = back[...]
    for one in started:
        one.wait_send()


def group_experts(outgoing, picks, joins, gate_weight, up_weight, down_weight):
    groups, room, width = outgoing.shape
    experts, _, hidden_width = gate_weight.shape
    pairs, pair_slots, pair_rows = picks.shape
    chunk = pair_slots // experts * 4
    out_width = down_weight.shape[2]
    part = (groups, 2, pair_rows, out_width)
    return pl.pallas_call(
        functools.partial(expert_kernel, groups),
        out_shape=jax.ShapeDtypeStruct(part, jnp.bfloat16),
        in_specs=[
            pl.BlockSpec(memory_space=pltpu.VMEM),
            pl.BlockSpec(memory_space=pltpu.VMEM),
            pl.BlockSpec(memory_space=pltpu.VMEM),
            pl.BlockSpec(memory_space=pl.ANY),
            pl.BlockSpec(memory_space=pl.ANY),
            pl.BlockSpec(memory_space=pl.ANY),
        ],
        out_specs=pl.BlockSpec(memory_space=pltpu.VMEM),
        scratch_shapes=[
            pltpu.VMEM((pairs, pair_rows, width), jnp.bfloat16),
            pltpu.VMEM((experts, chunk, width), jnp.bfloat16),
            pltpu.VMEM(gate_weight.shape, jnp.bfloat16),
            pltpu.VMEM(up_weight.shape, jnp.bfloat16),
            pltpu.VMEM(down_weight.shape, jnp.bfloat16),
            pltpu.VMEM((groups, 4, experts, chunk, hidden_width), jnp.bfloat16),
            pltpu.VMEM((4, pair_slots, out_width), jnp.bfloat16),
            pltpu.VMEM((2,) + part[1:], jnp.float32),
            pltpu.VMEM(part, jnp.bfloat16),
            pltpu.VMEM(part, jnp.bfloat16),
            pltpu.VMEM(part, jnp.bfloat16),
            pltpu.VMEM(part, jnp.bfloat16),
            pltpu.SemaphoreType.DMA((3,)),
            pltpu.SemaphoreType.DMA,
            pltpu.SemaphoreType.DMA((15, groups)),
            pltpu.SemaphoreType.DMA((15, groups)),
        ],
        compiler_params=pltpu.CompilerParams(
            collective_id=0, has_side_effects=True, vmem_limit_bytes=63 * 1024 * 1024
        ),
    )(outgoing, picks, joins, gate_weight, up_weight, down_weight)


def spread_kernel(count, own_ref, every_ref, held, send_sem, recv_sem):
    sp = lax.axis_index("sp")
    tp = lax.axis_index("tp")
    barrier = pltpu.get_barrier_semaphore()
    for k in range(1, count):
        device = (lax.rem(sp + k, count), tp)
        pl.semaphore_signal(barrier, inc=1, device_id=device, device_id_type=MESH)
    pl.semaphore_wait(barrier, count - 1)

    def copy(slot, device, k):
        return pltpu.make_async_remote_copy(
            src_ref=own_ref,
            dst_ref=held.at[slot],
            send_sem=send_sem.at[k],
            recv_sem=recv_sem.at[k],
            device_id=device,
            device_id_type=MESH,
        )

    copies = [copy(sp, (lax.rem(sp + k, count), tp), k) for k in range(1, count)]
    for one in copies:
        one.start()
    held[sp] = own_ref[...]
    for k in range(1, count):
        source = lax.rem(sp + count - k, count)
        copy(source, (source, tp), k).wait_recv()
    every_ref[...] = held[...]
    for one in copies:
        one.wait_send()


def spread(own):
    count = lax.axis_size("sp")
    shape = (count,) + own.shape
    return pl.pallas_call(
        functools.partial(spread_kernel, count),
        out_shape=jax.ShapeDtypeStruct(shape, own.dtype),
        in_specs=[pl.BlockSpec(memory_space=pltpu.VMEM)],
        out_specs=pl.BlockSpec(memory_space=pltpu.VMEM),
        scratch_shapes=[
            pltpu.VMEM(shape, own.dtype),
            pltpu.SemaphoreType.DMA((count,)),
            pltpu.SemaphoreType.DMA((count,)),
        ],
        compiler_params=pltpu.CompilerParams(collective_id=1, has_side_effects=True),
    )(own)


def group_ranks(mine):
    count = mine.astype(jnp.int32)
    return jnp.cumsum(count, 1) - count


def experts_by_group(
    normed, group, member, route_weight, gate_weight, up_weight, down_weight, capacity
):
    sp_size, tp_size = lax.axis_size("sp"), lax.axis_size("tp")
    row_count = normed.shape[0]
    block_rows = row_count // tp_size
    experts_local = gate_weight.shape[0]
    groups = experts_local * sp_size // PER_GROUP
    room = capacity * PER_GROUP // member.shape[1]
    packed = (group * PER_GROUP + member[:, 0]) * PER_GROUP + member[:, 1]
    facts = jnp.concatenate([packed.astype(jnp.float32)[None], route_weight.T], 0)
    facts = spread(jnp.pad(facts, ((0, 5), (0, 0))))
    every = facts[:, 0].astype(jnp.int32).reshape(-1, block_rows)
    own_group = lax.axis_index("sp") * experts_local // PER_GROUP
    first_expert = lax.axis_index("sp") * experts_local % PER_GROUP
    mine = every // (PER_GROUP * PER_GROUP) == own_group
    at = group_ranks(mine)
    names = [every // PER_GROUP % PER_GROUP, every % PER_GROUP]
    local = first_expert + jnp.arange(experts_local)[None, :, None]
    named = ((names[0][:, None, :] == local) | (names[1][:, None, :] == local)) & mine[:, None, :]
    slot = jnp.cumsum(named.astype(jnp.int32), 2) - 1
    slot = jnp.where(named, slot, -1)
    blocks = every.shape[0]
    slot_hot = (slot[:, :, None, :] == jnp.arange(capacity)[None, None, :, None]).astype(jnp.bfloat16)
    row_hot = (
        (at[:, :, None] == jnp.arange(room)[None, None, :]) & mine[:, :, None]
    ).astype(jnp.bfloat16)
    pick = jnp.einsum(
        "bsr,brg->bsg",
        slot_hot.reshape(blocks, experts_local * capacity, block_rows),
        row_hot,
        preferred_element_type=jnp.float32,
    ).astype(jnp.bfloat16)
    pick = pick.reshape(blocks // 2, 2, experts_local, capacity, room).transpose(0, 2, 1, 3, 4)
    both = jnp.eye(2, dtype=jnp.bfloat16)[None, None, :, None, :, None] * pick[:, :, :, :, None, :]
    picks = both.reshape(blocks // 2, experts_local * 2 * capacity, 2 * room)
    routes = facts[:, 1:3].transpose(1, 0, 2).reshape(2, blocks, 1, block_rows)
    routed = jnp.where(names[0][:, None, :] == local, routes[0], routes[1])
    slot_weight = jnp.sum(slot_hot.astype(jnp.float32) * routed[:, :, None, :], 3)
    slot_weight = slot_weight.reshape(blocks // 2, 2, experts_local, capacity)
    slot_weight = slot_weight.transpose(0, 2, 1, 3).reshape(blocks // 2, 1, -1)
    coarse = slot_weight.astype(jnp.bfloat16)
    fine = (slot_weight - coarse.astype(jnp.float32)).astype(jnp.bfloat16)
    joins = picks.transpose(0, 2, 1)[None] * jnp.stack([coarse, fine])
    by_block = group.reshape(tp_size, block_rows)
    group_mask = by_block[:, None, :] == jnp.arange(groups)[None, :, None]
    count = group_mask.astype(jnp.int32)
    place = jnp.cumsum(count, 2) - count
    choose = (
        (place[:, :, None, :] == jnp.arange(room)[None, None, :, None]) & group_mask[:, :, None, :]
    ).astype(jnp.bfloat16)
    choose = choose.reshape(tp_size, groups * room, block_rows)
    own_choose = lax.dynamic_index_in_dim(choose, lax.axis_index("tp"), 0, keepdims=False)
    own_rows = lax.dynamic_slice_in_dim(normed, lax.axis_index("tp") * block_rows, block_rows, 0)
    outgoing = jnp.dot(own_choose, own_rows, preferred_element_type=jnp.float32)
    outgoing = outgoing.astype(jnp.bfloat16).reshape(groups, room, normed.shape[1])
    back = group_experts(outgoing, picks, joins, gate_weight, up_weight, down_weight)
    back = back.reshape(groups, tp_size, room, -1).transpose(1, 0, 2, 3)
    back = back.reshape(tp_size, groups * room, -1)
    combined = jnp.einsum("tgr,tgc->trc", choose, back, preferred_element_type=jnp.float32)
    return combined.reshape(row_count, -1)


def shards(
    residual,
    queries,
    keys,
    values,
    segments,
    sink,
    out_weight,
    norm_gain_one,
    group,
    member,
    route_weight,
    gate_weight,
    up_weight,
    down_weight,
    norm_gain_two,
):
    row_count = queries.shape[0]
    sp_size = lax.axis_size("sp")
    tp_size = lax.axis_size("tp")
    kv_local = keys.shape[1] // HEAD_DIM
    heads_local = queries.shape[1] // HEAD_DIM
    group_size = heads_local // kv_local
    seq_total = row_count * sp_size
    seq_start = lax.axis_index("sp") * row_count
    joined = jnp.concatenate([keys, values], axis=1)
    padded, seg_padded = (
        with_halo(joined, (("sp", 0),), HALF),
        with_halo(segments, (("sp", 0),), HALF),
    )
    query_block = math.gcd(row_count, 512)
    key_span = query_block + 2 * HALF
    offsets = jnp.arange(key_span)[None, :] - HALF - jnp.arange(query_block)[:, None]
    in_band = jnp.abs(offsets) <= HALF
    sink_heads = sink.reshape(kv_local, group_size, 1, 1)
    query_heads = queries.reshape(row_count, kv_local, group_size, HEAD_DIM)
    key_cols = kv_local * HEAD_DIM
    pieces = []
    for number in range(row_count // query_block):
        row_low = number * query_block
        query_rows = query_heads[row_low : row_low + query_block]
        kv_rows = padded[row_low : row_low + key_span]
        key_part = kv_rows[:, :key_cols].reshape(key_span, kv_local, HEAD_DIM)
        value_part = kv_rows[:, key_cols:].reshape(key_span, kv_local, HEAD_DIM)
        key_place = seq_start + row_low - HALF + jnp.arange(key_span)
        inside = (key_place >= 0) & (key_place < seq_total)
        same_doc = (
            segments[row_low : row_low + query_block, None]
            == seg_padded[None, row_low : row_low + key_span]
        )
        allowed = in_band & same_doc & inside[None, :]
        scores = jnp.einsum(
            "qkgd,ckd->kgqc", query_rows, key_part, preferred_element_type=jnp.float32
        ) * HEAD_DIM ** (-0.5)
        masked = jnp.where(allowed, scores, -1e30)
        peak = jnp.maximum(jnp.max(masked, -1, keepdims=True), sink_heads)
        raised = jnp.where(allowed, jnp.exp(masked - peak), 0.0)
        denominator = jnp.sum(raised, -1, keepdims=True) + jnp.exp(sink_heads - peak)
        weights = (raised / denominator).astype(jnp.bfloat16)
        attended_part = jnp.einsum(
            "kgqc,ckd->qkgd", weights, value_part, preferred_element_type=jnp.float32
        )
        pieces.append(
            attended_part.reshape(query_block, heads_local * HEAD_DIM).astype(jnp.bfloat16)
        )
    attended = jnp.concatenate(pieces, 0)
    width = out_weight.shape[1]
    weight_rows = out_weight
    mixed = jnp.dot(
        lax.all_gather(attended, "tp", axis=1, tiled=True),
        weight_rows,
        preferred_element_type=jnp.float32,
    )
    pre_one = ALPHA * residual.astype(jnp.float32) + mixed
    normed = layer_norm(pre_one, norm_gain_one)
    experts_local = gate_weight.shape[0]
    expert_count = experts_local * sp_size
    picks_count = member.shape[1]
    block_rows = row_count // tp_size
    capacity = max(2, block_rows // 8)
    column_width = down_weight.shape[2]
    if experts_local * 2 == PER_GROUP and tp_size == 4:
        combined = experts_by_group(
            normed, group, member, route_weight, gate_weight, up_weight, down_weight, capacity
        )
    else:
        expert_ids = (group[:, None] * PER_GROUP + member).reshape(tp_size, block_rows * picks_count)
        onehot_table = (expert_ids[:, :, None] == jnp.arange(expert_count)[None, None, :]).astype(
            jnp.int32
        )
        ranks = jnp.sum((jnp.cumsum(onehot_table, 1) - 1) * onehot_table, 2)
        owner = expert_ids // experts_local
        local_ids = expert_ids % experts_local
        block_ids = jnp.arange(tp_size)[:, None]
        slot_all = ((local_ids * sp_size + owner) * tp_size + block_ids) * capacity + ranks
        copy_rows = (
            jnp.arange(row_count * picks_count).reshape(tp_size, block_rows * picks_count)
            // picks_count
        )
        extended = jnp.concatenate([normed, jnp.zeros((1, width), jnp.bfloat16)], 0)
        tp_place = lax.axis_index("tp")
        slot_own_base = (local_ids * sp_size + owner) * capacity + ranks
        own_slots = lax.dynamic_index_in_dim(slot_own_base, tp_place, 0, keepdims=False)
        own_rows = lax.dynamic_index_in_dim(copy_rows, tp_place, 0, keepdims=False)
        slot_count = experts_local * sp_size * capacity
        source = jnp.full((slot_count,), row_count, jnp.int32).at[own_slots].set(own_rows)
        outgoing = extended[source].reshape(experts_local, sp_size, capacity, width)
        received = lax.all_to_all(outgoing, "sp", split_axis=1, concat_axis=1, tiled=True)
        arrived = lax.all_gather(received, "tp", axis=2, tiled=True)
        expert_rows = arrived.reshape(experts_local, sp_size * tp_size * capacity, width)
        gate_part = jnp.einsum(
            "esd,edf->esf", expert_rows, gate_weight, preferred_element_type=jnp.float32
        )
        up_part = jnp.einsum("esd,edf->esf", expert_rows, up_weight, preferred_element_type=jnp.float32)
        hidden = (jax.nn.silu(gate_part) * up_part).astype(jnp.bfloat16)
        weight_rows = down_weight
        produced = jnp.einsum(
            "esf,efc->esc",
            lax.all_gather(hidden, "tp", axis=2, tiled=True),
            weight_rows,
            preferred_element_type=jnp.float32,
        ).astype(jnp.bfloat16)
        returned = lax.all_to_all(
            produced.reshape(experts_local, sp_size, tp_size * capacity, column_width),
            "sp",
            split_axis=1,
            concat_axis=1,
            tiled=True,
        )
        result_rows = returned.reshape(-1, column_width)
        picked = result_rows[slot_all.reshape(row_count, picks_count)]
        combined = jnp.sum(route_weight[:, :, None] * picked.astype(jnp.float32), 1)
    column_start = lax.axis_index("tp") * column_width
    normed_part = lax.dynamic_slice_in_dim(normed, column_start, column_width, 1)
    pre_two = ALPHA * normed_part.astype(jnp.float32) + combined
    sums, squares = lax.psum((jnp.sum(pre_two, -1), jnp.sum(pre_two * pre_two, -1)), "tp")
    mean_value = (sums / width)[:, None]
    variance = (squares / width)[:, None] - mean_value * mean_value
    return ((pre_two - mean_value) * lax.rsqrt(variance + EPS) * norm_gain_two).astype(jnp.bfloat16)


def solution(mesh):
    in_specs = (
        P("sp", None),
        P("sp", "tp"),
        P("sp", "tp"),
        P("sp", "tp"),
        P("sp"),
        P("tp"),
        P(),
        P(),
        P("sp"),
        P("sp", None),
        P("sp", None),
        P("sp", None, "tp"),
        P("sp", None, "tp"),
        P("sp", None, "tp"),
        P("tp"),
    )
    out_specs = P("sp", "tp")
    return jax.shard_map(shards, mesh=mesh, in_specs=in_specs, out_specs=out_specs, check_vma=False)
```
